256 devices in a mesh: kv: 32 (over z, x), tp: 8 (over y, core).
Axes of the slice: x: 4, y: 4, z: 8, core: 2. Of those that a mesh axis runs over, the one named last changes fastest.
Arguments:
- tokens: bfloat16 [16, 2048], P(None, ('kv', 'tp')), may hold values from -60 to 60, as said below
- w_query: bfloat16 [2048, 1024], P('kv', 'tp'), may hold values from -0.125 to 0.125
- w_key: bfloat16 [2048, 1024], P('kv', 'tp'), may hold values from -0.125 to 0.125
- w_value: bfloat16 [2048, 1024], P('kv', 'tp'), may hold values from -0.125 to 0.125
- w_forget: bfloat16 [2048, 8], replicated, may hold values from -0.125 to 0.125
- w_out: bfloat16 [1024, 2048], P('tp', 'kv'), may hold values from -1 to 1, as said below
- mix_gain: float32 [2048], P(('kv', 'tp')), may hold values from 0.1 to 1.9
- mix_bias: float32 [2048], P(('kv', 'tp')), may hold values from -3 to 3
- ffn_gain: float32 [2048], P(('kv', 'tp')), may hold values from 0.1 to 1.9
- ffn_bias: float32 [2048], P(('kv', 'tp')), may hold values from -3 to 3
- w_up: bfloat16 [2048, 8192], P('kv', 'tp'), may hold values from -0.125 to 0.125
- down_weight: bfloat16 [8192, 2048], P('tp', 'kv'), may hold values from -0.5 to 0.5, as said below
- cache_keys: bfloat16 [16, 8, 16384, 128], P(None, 'tp', 'kv'), may hold values from -200 to 200, as said below
- cache_values: bfloat16 [16, 8, 16384, 128], P(None, 'tp', 'kv'), may hold values from -24 to 24
- cum_gates: float32 [16, 8, 16384], P(None, 'tp', 'kv'), as said below
Outputs:
- result: bfloat16 [16, 2048], P(None, ('kv', 'tp'))
The draws below stay inside these ranges and needn't reach their ends.
Inputs may be any that keep to these rules, and one draw needn't show every extreme that they name: `tokens`: real-valued rows. `cache_keys`: real-valued keys. `cum_gates`: sums of log gates. `w_out`: real-valued weights. `down_weight`: real-valued weights.
All inputs are finite; a program needn't handle non-finite values.
Results may differ from the reference program's by a relative error of at most 0.0075.
Values may be sent and summed in bfloat16 or wider, within the bound.
A program may use at most 64 MiB of HBM per device.

```python
import jax
import jax.numpy as jnp
from jax import lax

D = 2048
ATTENTION_COUNT = 8
HEAD_DIM = 128
FF = 8192
SEQUENCE_COUNT = 16
POS_DEV = 512
LENGTH = 16384
N_KV = 32


def draw_tokens(key, part):
    key_base, key_rough = jax.random.split(key, 2)
    columns = jnp.arange(D, dtype=jnp.float32) / D
    rough = jnp.exp(jax.random.uniform(key_rough, (D,), jnp.float32, -0.7, 0.7))
    col_scale = 3.0 ** columns * rough
    base = jnp.clip(jax.random.normal(key_base, (SEQUENCE_COUNT, D), jnp.float32), -6.0, 6.0)
    return (base * col_scale).astype(jnp.bfloat16)


def column_pattern(key, width):
    key_sign, key_size = jax.random.split(key, 2)
    sign_pattern = (2 * jax.random.randint(key_sign, (1, width), 0, 2) - 1).astype(jnp.float32)
    magnitude = jax.random.uniform(key_size, (1, width), jnp.float32, 0.5, 1.5)
    return sign_pattern * magnitude


def draw_w_out(key, part):
    key_base, key_pattern = jax.random.split(key, 2)
    row_count = ATTENTION_COUNT * HEAD_DIM
    fan_scale = float(row_count) ** (-0.5)
    pattern = column_pattern(key_pattern, D)
    base_part = jnp.clip(jax.random.normal(key_base, (row_count, D), jnp.float32), -6.0, 6.0)
    return ((base_part + pattern) * fan_scale).astype(jnp.bfloat16)


def draw_down_weight(key, part):
    key_base, key_pattern = jax.random.split(key, 2)
    fan_scale = float(FF) ** (-0.5)
    pattern = column_pattern(key_pattern, D)
    base_part = jnp.clip(jax.random.normal(key_base, (FF, D), jnp.float32), -6.0, 6.0)
    common_share = 2.0
    return (base_part * fan_scale + common_share * pattern / float(FF)).astype(jnp.bfloat16)


def draw_cache_keys(key, part):
    key_base = jax.random.fold_in(key, 0)
    shape = (SEQUENCE_COUNT, ATTENTION_COUNT, LENGTH, HEAD_DIM)
    base = jnp.clip(jax.random.normal(key_base, shape, jnp.float32), -6.0, 6.0)
    return base.astype(jnp.bfloat16)


def draw_cum_gates(key, part):
    lookup_vectors = jax.random.split(key, 7)
    slow_share = 0.5
    slow_heads = jax.random.uniform(lookup_vectors[0], (1, ATTENTION_COUNT, 1), jnp.float32) < slow_share
    gradual_fading_factor = 0.5 / LENGTH * jnp.exp(jax.random.uniform(lookup_vectors[1], (1, ATTENTION_COUNT, 1), jnp.float32, -0.5, 0.5))
    fast_rate = 1.0 / 50.0 * jnp.exp(jax.random.uniform(lookup_vectors[2], (1, ATTENTION_COUNT, 1), jnp.float32, -0.5, 0.5))
    head_rate = jnp.where(slow_heads, gradual_fading_factor, fast_rate)
    block_factor = 2.0 ** jax.random.uniform(lookup_vectors[3], (N_KV,), jnp.float32, -1.5, 1.5)
    block_factor = jnp.repeat(block_factor, POS_DEV)
    rough = jax.random.uniform(lookup_vectors[4], (SEQUENCE_COUNT, ATTENTION_COUNT, LENGTH), jnp.float32, 0.3, 1.7)
    retention_exponent_terms = -head_rate * block_factor[None, None, :] * rough
    place_indices = jax.random.randint(lookup_vectors[5], (SEQUENCE_COUNT, 1, 3), 0, LENGTH)
    cache_places = jnp.arange(LENGTH, dtype=jnp.int32)
    abrupt_jump_occurrences = jnp.any(cache_places[None, None, None, :] == place_indices[..., None], axis=2)
    memory_loss_levels = jnp.log(jax.random.uniform(lookup_vectors[6], (SEQUENCE_COUNT, ATTENTION_COUNT, 1), jnp.float32, 0.5, 0.8))
    retention_exponent_terms = retention_exponent_terms + jnp.where(abrupt_jump_occurrences, memory_loss_levels, 0.0)
    subsequent_accumulation = jnp.cumsum(retention_exponent_terms[..., ::-1], axis=-1)[..., ::-1] - retention_exponent_terms
    return subsequent_accumulation.astype(jnp.float32)


def level_of(own_key, shape, cuts, least, high):
    level, own = 1.0, jax.random.fold_in(own_key, 6)
    for position, shards_of in cuts:
        heights = jnp.exp(jax.random.uniform(jax.random.fold_in(own, position), (shards_of,), jnp.float32, least / len(cuts), high / len(cuts)))
        level = level * jnp.repeat(heights, shape[position] // shards_of).reshape([-1 if axis == position else 1 for axis in range(len(shape))])
    return level


def centred(own_key, dims, spread, reach, cuts=(), held_as=jnp.bfloat16):
    drawn = jax.random.normal(own_key, dims, jnp.float32) * spread
    if len(cuts) > 0:
        drawn = level_of(own_key, dims, cuts, -0.22, 0.18) * drawn
    return jnp.clip(drawn, min=-reach, max=reach).astype(held_as)


def setup_inputs(seed: int = 0) -> dict:
    key_of = jax.random.split(jax.random.key(seed), 16)
    return {
        "tokens": draw_tokens(jax.random.fold_in(key_of[15], 71), 0),
        "w_query": centred(key_of[1], (D, ATTENTION_COUNT * HEAD_DIM), D ** -0.5, 0.125, ((0, 32), (1, 8))),
        "w_key": centred(key_of[2], (D, ATTENTION_COUNT * HEAD_DIM), D ** -0.5, 0.125, ((0, 32), (1, 8))),
        "w_value": centred(key_of[3], (D, ATTENTION_COUNT * HEAD_DIM), D ** -0.5, 0.125, ((0, 32), (1, 8))),
        "w_forget": centred(key_of[4], (D, ATTENTION_COUNT), D ** -0.5, 0.125),
        "w_out": draw_w_out(jax.random.fold_in(key_of[15], 71), 0),
        "mix_gain": jnp.clip(1.0 + 0.18 * jax.random.normal(key_of[6], (D,), jnp.float32), 0.1, 1.9),
        "mix_bias": centred(key_of[7], (D,), 0.5, 3.0, ((0, 256),), jnp.float32),
        "ffn_gain": jnp.clip(1.0 + 0.18 * jax.random.normal(key_of[8], (D,), jnp.float32), 0.1, 1.9),
        "ffn_bias": centred(key_of[9], (D,), 0.5, 3.0, ((0, 256),), jnp.float32),
        "w_up": centred(key_of[10], (D, FF), D ** -0.5, 0.125, ((0, 32), (1, 8))),
        "down_weight": draw_down_weight(jax.random.fold_in(key_of[15], 71), 0),
        "cache_keys": draw_cache_keys(jax.random.fold_in(key_of[15], 71), 0),
        "cache_values": centred(key_of[13], (SEQUENCE_COUNT, ATTENTION_COUNT, LENGTH, HEAD_DIM), 4.0, 24.0, ((1, 8), (2, 32))),
        "cum_gates": draw_cum_gates(jax.random.fold_in(key_of[15], 71), 0),
    }


residual_scale = 1.4142135623730951
norm_eps = 1e-05

def layer_norm(residual_sum, gain, bias):
    row_mean = lax.optimization_barrier(jnp.mean(residual_sum, axis=-1, keepdims=True))
    row_var = lax.optimization_barrier(jnp.mean(residual_sum * residual_sum, axis=-1, keepdims=True)) - row_mean * row_mean
    return (residual_sum - row_mean) * lax.rsqrt(row_var + norm_eps) * gain + bias

def reference(tokens, w_query, w_key, w_value, w_forget, w_out, mix_gain, mix_bias, ffn_gain, ffn_bias, w_up, down_weight, cache_keys, cache_values, cum_gates):
    batch_entries = tokens.shape[0]
    query = jnp.dot(tokens, w_query, preferred_element_type=jnp.float32).astype(jnp.bfloat16)
    key_new = jnp.dot(tokens, w_key, preferred_element_type=jnp.float32).astype(jnp.bfloat16)
    value_new = jnp.dot(tokens, w_value, preferred_element_type=jnp.float32).astype(jnp.bfloat16)
    log_forget = jax.nn.log_sigmoid(jnp.dot(tokens, w_forget, preferred_element_type=jnp.float32))
    query_heads = query.reshape(batch_entries, ATTENTION_COUNT, HEAD_DIM).astype(jnp.float32)
    key_heads = key_new.reshape(batch_entries, ATTENTION_COUNT, HEAD_DIM).astype(jnp.float32)
    value_heads = value_new.reshape(batch_entries, ATTENTION_COUNT, HEAD_DIM).astype(jnp.float32)
    score_scale = HEAD_DIM ** (-0.5)

    def one_block(block_index):
        block_start = (block_index * POS_DEV).astype(jnp.int32)
        key_block = lax.dynamic_slice_in_dim(cache_keys, block_start, POS_DEV, 2).astype(jnp.float32)
        value_block = lax.dynamic_slice_in_dim(cache_values, block_start, POS_DEV, 2).astype(jnp.float32)
        gate_block = lax.dynamic_slice_in_dim(cum_gates, block_start, POS_DEV, 2)
        scores = jnp.einsum('bhd,bhpd->bhp', query_heads, key_block) * score_scale + gate_block + log_forget[:, :, None]
        peak_score = lax.optimization_barrier(jnp.max(scores, axis=-1))
        weights = jnp.exp(scores - peak_score[..., None])
        weight_total = lax.optimization_barrier(jnp.sum(weights, axis=-1))
        rounded = lax.optimization_barrier(weights.astype(jnp.bfloat16))
        weighted = jnp.einsum('bhp,bhpd->bhd', rounded.astype(jnp.float32), value_block)
        return (peak_score, weight_total, weighted)
    peaks, totals, accums = lax.map(one_block, jnp.arange(N_KV, dtype=jnp.int32))
    own_score = lax.optimization_barrier(jnp.sum(query_heads * key_heads, axis=-1)) * score_scale
    peak_all = jnp.maximum(lax.optimization_barrier(jnp.max(peaks, axis=0)), own_score)
    factors = jnp.exp(peaks - peak_all[None])
    own_factor = jnp.exp(own_score - peak_all)
    denom = lax.optimization_barrier(jnp.sum(factors * totals, axis=0)) + own_factor
    numer = lax.optimization_barrier(jnp.sum(factors[..., None] * accums, axis=0)) + own_factor[..., None] * value_heads
    attended = (numer / denom[..., None]).astype(jnp.bfloat16).reshape(batch_entries, ATTENTION_COUNT * HEAD_DIM)
    mixed = residual_scale * tokens.astype(jnp.float32) + jnp.dot(attended, w_out, preferred_element_type=jnp.float32)
    normed = layer_norm(mixed, mix_gain, mix_bias).astype(jnp.bfloat16)
    up_proj = jnp.dot(normed, w_up, preferred_element_type=jnp.float32)
    hidden = jnp.square(jax.nn.relu(up_proj)).astype(jnp.bfloat16)
    outer = residual_scale * normed.astype(jnp.float32) + jnp.dot(hidden, down_weight, preferred_element_type=jnp.float32)
    return layer_norm(outer, ffn_gain, ffn_bias).astype(jnp.bfloat16)
```

```python
import jax
import jax.numpy as jnp
from jax import lax
from jax.experimental import pallas as pl
from jax.experimental.pallas import tpu as pltpu
from jax.sharding import Mesh
from jax.sharding import PartitionSpec as P

D = 2048
HEAD_DIM = 128
B = 16
POS = 512
NZ, NX, NY, NC = 8, 4, 4, 2
NKV, NTP = NZ * NX, NY * NC
ROOT2 = 1.4142135623730951
EPS = 1e-05
SCALE = HEAD_DIM**-0.5
F32 = jnp.float32
BF16 = jnp.bfloat16
MESH = pl.DeviceIdType.MESH


def body(
    tokens, w_query, w_key, w_value, w_forget, w_out, mix_gain, mix_bias, ffn_gain, ffn_bias,
    w_up, w_down, keys, values, gates,
    out,
    tok_v, gain_v, bias_v, fgain_v, fbias_v, wq_v, wkv_v, wf_v, wo_v, wup_v, wdn_v, k_v, v_v, cg_v,
    stage, plane, q_buf, kvg_send, kvg_buf, gwb_send, gwb_buf, accx, stx, accz, stz, head_buf,
    mst, up_send, up_buf, hid_buf, hid_f, down_buf, ost,
    load_sem, k_sem, v_sem, send_sem, recv_sem,
):
    z, x, y, c = (lax.axis_index(a) for a in ("z", "x", "y", "c"))
    kv = z * NX + x
    tp = y * NC + c
    slot = x * NTP + tp

    barrier = pltpu.get_barrier_semaphore()

    def plane_peer(i):
        t = i // NTP
        r = i % NTP
        px = (x + NX - 1 - t + NX) % NX
        py = (y + NY - 1 - r // NC + NY) % NY
        pc = (c + NC - 1 - r % NC) % NC
        return {"x": px, "y": py, "c": pc}

    def greet_plane(i, carry):
        pl.semaphore_signal(barrier, inc=1, device_id=plane_peer(i), device_id_type=MESH)
        return carry

    def greet_line(i, carry):
        pl.semaphore_signal(
            barrier, inc=1, device_id={"z": (z + 1 + i) % NZ}, device_id_type=MESH
        )
        return carry

    lax.fori_loop(0, NZ - 1, greet_line, 0)
    lax.fori_loop(0, NX * NTP - 1, greet_plane, 0)

    loads = []

    def load(src, dst, sem):
        copy = pltpu.make_async_copy(src, dst, sem)
        copy.start()
        return copy

    first = [
        load(tokens, tok_v, load_sem.at[0]),
        load(mix_gain, gain_v, load_sem.at[1]),
        load(mix_bias, bias_v, load_sem.at[2]),
    ]
    load_q = load(w_query, wq_v.at[x], load_sem.at[3])
    load_k = load(w_key, wkv_v.at[x, 0], load_sem.at[4])
    load_v = load(w_value, wkv_v.at[x, 1], load_sem.at[5])
    load_f = load(w_forget.at[pl.ds(z * NX * 64, NX * 64)], wf_v, load_sem.at[6])
    load_o = load(w_out, wo_v, load_sem.at[7])
    load_up = load(w_up, wup_v, load_sem.at[8])
    load_fg = load(ffn_gain, fgain_v, load_sem.at[9])
    load_fb = load(ffn_bias, fbias_v, load_sem.at[10])
    load_cg = load(gates, cg_v, load_sem.at[11])
    load_key = [load(keys.at[pl.ds(4 * i, 4)], k_v.at[pl.ds(4 * i, 4)], k_sem.at[i]) for i in range(4)]
    load_val = [load(values.at[pl.ds(4 * i, 4)], v_v.at[pl.ds(4 * i, 4)], v_sem.at[i]) for i in range(4)]
    load_dn = load(w_down, wdn_v, load_sem.at[12])

    lane = lax.broadcasted_iota(jnp.int32, (B, 128), 1)
    row = lax.broadcasted_iota(jnp.int32, (B, 128), 0)
    lane1 = lax.broadcasted_iota(jnp.int32, (1, 128), 1)
    diag = row == lane
    diag16 = row == lane - B

    def to_row(col, mask):
        return jnp.sum(jnp.where(mask, jnp.broadcast_to(col, (B, 128)), 0.0), axis=0, keepdims=True)

    def to_col(line):
        return jnp.sum(
            jnp.where(diag, jnp.broadcast_to(line, (B, 128)), 0.0), axis=1, keepdims=True
        )

    for copy in first:
        copy.wait()
    stage[...] = jnp.zeros((128, 128), F32)
    stage[0:B, 0:8] = tok_v[...].astype(F32)
    stage[B : B + 1, 0:8] = gain_v[...]
    stage[B + 1 : B + 2, 0:8] = bias_v[...]
    plane[slot] = stage[...].T[0:8, :]
    load_q.wait()
    load_k.wait()
    load_v.wait()

    pl.semaphore_wait(barrier, NZ - 1 + NX * NTP - 1)

    def push(src, dst, phase, peer):
        pltpu.make_async_remote_copy(
            src_ref=src,
            dst_ref=dst,
            send_sem=send_sem.at[phase],
            recv_sem=recv_sem.at[phase],
            device_id=peer,
            device_id_type=MESH,
        ).start()

    def received(ref, count, phase):
        part = ref.at[pl.ds(0, count)]
        pltpu.make_async_copy(part, part, recv_sem.at[phase]).wait()

    def sent(ref, count, phase):
        part = ref.at[pl.ds(0, count)]
        pltpu.make_async_copy(part, part, send_sem.at[phase]).wait()

    def line_peer(i):
        step = (i + 1) // 2 * (2 * (i % 2) - 1) + 4
        return (z + step + NZ) % NZ

    def kv_peer(i):
        t = i // NX
        step = (t + 1) // 2 * (2 * (t % 2) - 1) + 4
        return (z + step + NZ) % NZ, (x + NX - 1 - i % NX) % NX

    def loop(count, f):
        def step(i, carry):
            f(i)
            return carry

        lax.fori_loop(0, count, step, 0)

    loop(NX * NTP - 1, lambda i: push(plane.at[slot], plane.at[slot], 0, plane_peer(i)))
    loop(NX - 1, lambda i: push(wq_v.at[x], wq_v.at[x], 1, {"x": (x + NX - 1 - i) % NX}))
    loop(NX - 1, lambda i: push(wkv_v.at[x], wkv_v.at[x], 2, {"x": (x + NX - 1 - i) % NX}))

    received(plane, NX * NTP - 1, 0)
    spread = plane[...].reshape(NX * NTP * 8, 128).T
    tok = spread[0:B, :].astype(BF16)
    received(wq_v, NX - 1, 1)
    q_buf[z] = jnp.dot(tok, wq_v[...].reshape(NX * 64, HEAD_DIM), preferred_element_type=F32)
    loop(
        NZ - 1, lambda i: push(q_buf.at[z], q_buf.at[z], 3, {"z": line_peer(i)})
    )
    received(wkv_v, NX - 1, 2)
    load_f.wait()
    key_part = jnp.dot(tok, wkv_v[:, 0].reshape(NX * 64, HEAD_DIM), preferred_element_type=F32)
    value_part = jnp.dot(tok, wkv_v[:, 1].reshape(NX * 64, HEAD_DIM), preferred_element_type=F32)
    gate_part = jnp.dot(tok, wf_v[...], preferred_element_type=F32)
    lane8 = lax.broadcasted_iota(jnp.int32, (B, 8), 1)
    gate_part = jnp.sum(jnp.where(lane8 == tp, gate_part, 0.0), axis=1, keepdims=True)
    gate_part = jnp.broadcast_to(gate_part, (B, 128))
    for i in range(NZ):
        kvg_send[i, :, 0:128] = key_part[2 * i : 2 * i + 2, :]
        kvg_send[i, :, 128:256] = value_part[2 * i : 2 * i + 2, :]
        kvg_send[i, :, 256:384] = gate_part[2 * i : 2 * i + 2, :]
    kvg_buf[z] = kvg_send[z]

    def push_kvg(i):
        pz = line_peer(i)
        push(kvg_send.at[pz], kvg_buf.at[z], 4, {"z": pz})

    loop(NZ - 1, push_kvg)

    own = jnp.where(x >= 2, spread[0:24, 128:256], spread[0:24, 0:128])
    own = jnp.where(x % 2 == 1, pltpu.roll(own, 64, 1), own)
    tok_own = own[0:B, :]
    gain_own = own[B : B + 1, :]
    bias_own = own[B + 1 : B + 2, :]

    load_up.wait()
    both = jnp.concatenate([gain_own, bias_own], axis=0)[:, 0:64]
    both_hi = both.astype(BF16)
    both_lo = (both - both_hi.astype(F32)).astype(BF16)
    gwb = jnp.dot(
        jnp.concatenate([both_hi.astype(F32), both_lo.astype(F32)], axis=0).astype(BF16),
        wup_v[...],
        preferred_element_type=F32,
    )
    gwb = gwb[0:2, :] + gwb[2:4, :]
    for h in range(2):
        for j in range(4):
            at = (h * 4 + j) * 128
            gwb_send[h, j : j + 1, :] = gwb[0:1, at : at + 128]
            gwb_send[h, 4 + j : 5 + j, :] = gwb[1:2, at : at + 128]
    gwb_buf[kv] = gwb_send[kv % 2]

    received(q_buf, NZ - 1, 3)
    query = jnp.sum(q_buf[...], axis=0).astype(BF16)

    def push_gwb(i):
        pz, px = kv_peer(i)
        push(gwb_send.at[px % 2], gwb_buf.at[kv], 5, {"z": pz, "x": px})

    loop(NKV - 1, push_gwb)

    load_cg.wait()
    row_pos = lax.broadcasted_iota(jnp.int32, (B, POS), 0)
    scores = jnp.zeros((B, POS), F32)
    for b in range(B):
        if b % 4 == 0:
            load_key[b // 4].wait()
        part = lax.dot_general(
            query, k_v[b], (((1,), (1,)), ((), ())), preferred_element_type=F32
        )
        scores = jnp.where(row_pos == b, part, scores)
    gates_here = jnp.concatenate([cg_v[b] for b in range(B)], axis=0)
    scores = scores * SCALE + gates_here
    received(kvg_buf, NZ - 1, 4)
    kvg = jnp.sum(kvg_buf[...], axis=0)
    kvg16 = jnp.where(
        lax.broadcasted_iota(jnp.int32, (B, 384), 0) % 2 == 0,
        jnp.broadcast_to(kvg[0:1, :], (B, 384)),
        jnp.broadcast_to(kvg[1:2, :], (B, 384)),
    )
    key_new = kvg16[:, 0:128].astype(BF16).astype(F32)
    value_new = kvg16[:, 128:256].astype(BF16).astype(F32)
    gate_sum = kvg16[:, 256:257]
    log_forget = jnp.minimum(gate_sum, 0.0) - jnp.log1p(jnp.exp(-jnp.abs(gate_sum)))
    own_score = jnp.sum(query.astype(F32) * key_new, axis=1, keepdims=True) * SCALE - log_forget
    mine = (row[:, 0:1] // 2 == z) & (x == 0)
    own_score = jnp.where(mine, own_score, -1e30)
    value_new = jnp.where(mine, value_new, 0.0)
    peak = jnp.maximum(jnp.max(scores, axis=1, keepdims=True), own_score)
    weights = jnp.exp(scores - peak)
    own_weight = jnp.exp(own_score - peak)
    total = jnp.sum(weights, axis=1, keepdims=True) + own_weight
    weights = weights.astype(BF16)
    acc = jnp.zeros((B, HEAD_DIM), F32)
    for b in range(B):
        if b % 4 == 0:
            load_val[b // 4].wait()
        part = jnp.dot(weights, v_v[b], preferred_element_type=F32)
        acc = jnp.where(row == b, part, acc)
    acc = acc + own_weight * value_new

    stx[x] = jnp.concatenate([to_row(peak, diag), to_row(total, diag)], axis=0)
    loop(NX - 1, lambda i: push(stx.at[x], stx.at[x], 7, {"x": (x + NX - 1 - i) % NX}))
    accx[x] = acc
    loop(NX - 1, lambda i: push(accx.at[x], accx.at[x], 6, {"x": (x + NX - 1 - i) % NX}))

    def combine(acc_ref, st_ref, count, acc_phase, st_phase):
        received(st_ref, count - 1, st_phase)
        peaks = [st_ref[i, 0:1, :] for i in range(count)]
        peak = peaks[0]
        for p in peaks[1:]:
            peak = jnp.maximum(peak, p)
        factors = [jnp.exp(p - peak) for p in peaks]
        total = factors[0] * st_ref[0, 1:2, :]
        for i in range(1, count):
            total = total + factors[i] * st_ref[i, 1:2, :]
        cols = [to_col(f) for f in factors]
        received(acc_ref, count - 1, acc_phase)
        acc = cols[0] * acc_ref[0]
        for i in range(1, count):
            acc = acc + cols[i] * acc_ref[i]
        return peak, total, acc

    load_o.wait()
    w_out2 = jnp.concatenate([wo_v[...], wo_v[...]], axis=1)
    load_dn.wait()
    w_down2 = jnp.concatenate([wdn_v[...], wdn_v[...]], axis=1)

    peak, total, acc = combine(accx, stx, NX, 6, 7)
    stz[z] = jnp.concatenate([peak, total], axis=0)
    loop(NZ - 1, lambda i: push(stz.at[z], stz.at[z], 9, {"z": line_peer(i)}))
    accz[z] = acc
    loop(NZ - 1, lambda i: push(accz.at[z], accz.at[z], 8, {"z": line_peer(i)}))
    peak, total, acc = combine(accz, stz, NZ, 8, 9)
    attended = (acc / to_col(total)).astype(BF16)

    lane_half = lax.broadcasted_iota(jnp.int32, (8, 128), 1) < 64

    def tp_peer(i):
        return {"y": (y + NY - 1 - i // NC) % NY, "c": (c + NC - 1 - i % NC) % NC}

    def tp_sum(terms, ref, phase):
        ref[tp] = jnp.where(lane_half, terms[0:8, :], terms[8:16, :])
        loop(NTP - 1, lambda i: push(ref.at[tp], ref.at[tp], phase, tp_peer(i)))
        received(ref, NTP - 1, phase)
        summed = jnp.sum(ref[...], axis=0)
        return jnp.concatenate([summed, pltpu.roll(summed, 64, 1)], axis=0)

    head_terms = tp_sum(jnp.dot(attended, w_out2, preferred_element_type=F32), head_buf, 10)
    mixed = jnp.where(lane < 64, ROOT2 * tok_own + head_terms, 0.0)

    def push_stats(values, ref, phase):
        sums = jnp.sum(values, axis=1, keepdims=True)
        squares = jnp.sum(values * values, axis=1, keepdims=True)
        ref[kv] = to_row(sums, diag) + to_row(squares, diag16)

        def push_one(i):
            pz, px = kv_peer(i)
            push(ref.at[kv], ref.at[kv], phase, {"z": pz, "x": px})

        loop(NKV - 1, push_one)

    def stats(ref, phase):
        received(ref, NKV - 1, phase)
        line = jnp.sum(ref[...], axis=0)
        mean = line / D
        var = pltpu.roll(line, 128 - B, 1) / D - mean * mean
        return mean, lax.rsqrt(var + EPS)

    push_stats(mixed, mst, 11)

    scaled = mixed * jnp.broadcast_to(gain_own, (B, 128))
    scaled_hi = scaled.astype(BF16)
    scaled_lo = (scaled - scaled_hi.astype(F32)).astype(BF16)
    up = jnp.dot(
        jnp.concatenate([scaled_hi, scaled_lo], axis=0)[:, 0:64],
        wup_v[...],
        preferred_element_type=F32,
    )
    up = up[0:B, :] + up[B : 2 * B, :]
    for h in range(2):
        for j in range(4):
            at = (h * 4 + j) * 128
            up_send[:, h, j, :] = up[:, at : at + 128]
    up_buf[kv] = up_send[kv // 2, kv % 2]

    def push_up(i):
        pz, px = kv_peer(i)
        push(up_send.at[2 * pz + px // 2, px % 2], up_buf.at[kv], 12, {"z": pz, "x": px})

    loop(NKV - 1, push_up)
    received(gwb_buf, NKV - 1, 5)
    gwb = jnp.sum(gwb_buf[...], axis=0)
    mean, rstd = stats(mst, 11)
    pick = lane1 == kv // 2
    mean_here = jnp.sum(jnp.where(pick, mean, 0.0), axis=1, keepdims=True)
    rstd_here = jnp.sum(jnp.where(pick, rstd, 0.0), axis=1, keepdims=True)
    received(up_buf, NKV - 1, 12)
    up_sum = jnp.sum(up_buf[...], axis=0)
    up_row = rstd_here * (up_sum - mean_here * gwb[0:4, :]) + gwb[4:8, :]
    hidden = jnp.square(jnp.maximum(up_row, 0.0)).astype(BF16)
    hid_buf[kv] = hidden

    def push_hidden(i):
        pz, px = kv_peer(i)
        push(hid_buf.at[kv], hid_buf.at[kv], 13, {"z": pz, "x": px})

    loop(NKV - 1, push_hidden)

    normed = (mixed - to_col(mean)) * to_col(rstd) * gain_own + bias_own
    normed = normed.astype(BF16).astype(F32)
    fgain = fgain_v
    received(hid_buf, NKV - 1, 13)
    hid_f[...] = hid_buf[...].astype(F32).reshape(B, 2, 4, 128)
    hidden_all = jnp.concatenate(
        [hid_f[:, h, j, :].astype(BF16) for h in range(2) for j in range(4)], axis=1
    )
    down_terms = tp_sum(jnp.dot(hidden_all, w_down2, preferred_element_type=F32), down_buf, 14)
    outer = jnp.where(lane < 64, ROOT2 * normed + down_terms, 0.0)
    push_stats(outer, ost, 15)
    outer = pltpu.roll(outer, (128 - 8 * tp) % 128, 1)[:, 0:8]
    load_fg.wait()
    load_fb.wait()

    sent(plane, NX * NTP - 1, 0)
    sent(wq_v, NX - 1, 1)
    sent(wkv_v, NX - 1, 2)
    sent(q_buf, NZ - 1, 3)
    sent(kvg_buf, NZ - 1, 4)
    sent(gwb_buf, NKV - 1, 5)
    sent(accx, NX - 1, 6)
    sent(stx, NX - 1, 7)
    sent(accz, NZ - 1, 8)
    sent(stz, NZ - 1, 9)
    sent(head_buf, NTP - 1, 10)
    sent(mst, NKV - 1, 11)
    sent(up_buf, NKV - 1, 12)
    sent(hid_buf, NKV - 1, 13)
    sent(down_buf, NTP - 1, 14)
    sent(ost, NKV - 1, 15)
    mean, rstd = stats(ost, 15)
    result = (outer - to_col(mean)) * to_col(rstd) * fgain_v[...] + fbias_v[...]
    out[...] = result.astype(BF16)


def shards(
    tokens, w_query, w_key, w_value, w_forget, w_out, mix_gain, mix_bias, ffn_gain, ffn_bias,
    w_up, down_weight, cache_keys, cache_values, cum_gates,
):
    vmem = pltpu.VMEM
    scratch = [
        vmem((B, 8), BF16),
        vmem((1, 8), F32),
        vmem((1, 8), F32),
        vmem((1, 8), F32),
        vmem((1, 8), F32),
        vmem((NX, 64, 128), BF16),
        vmem((NX, 2, 64, 128), BF16),
        vmem((NX * 64, 8), BF16),
        vmem((128, 64), BF16),
        vmem((64, 1024), BF16),
        vmem((1024, 64), BF16),
        vmem((B, POS, 128), BF16),
        vmem((B, POS, 128), BF16),
        vmem((B, 1, POS), F32),
        vmem((128, 128), F32),
        vmem((NX * NTP, 8, 128), F32),
        vmem((NZ, B, 128), F32),
        vmem((NZ, 2, 384), F32),
        vmem((NZ, 2, 384), F32),
        vmem((2, 8, 128), F32),
        vmem((NKV, 8, 128), F32),
        vmem((NX, B, 128), F32),
        vmem((NX, 2, 128), F32),
        vmem((NZ, B, 128), F32),
        vmem((NZ, 2, 128), F32),
        vmem((NTP, 8, 128), F32),
        vmem((NKV, 1, 128), F32),
        vmem((B, 2, 4, 128), F32),
        vmem((NKV, 4, 128), F32),
        vmem((NKV, 4, 128), BF16),
        vmem((B, 2, 4, 128), F32),
        vmem((NTP, 8, 128), F32),
        vmem((NKV, 1, 128), F32),
        pltpu.SemaphoreType.DMA((13,)),
        pltpu.SemaphoreType.DMA((4,)),
        pltpu.SemaphoreType.DMA((4,)),
        pltpu.SemaphoreType.DMA((16,)),
        pltpu.SemaphoreType.DMA((16,)),
    ]
    any_space = pl.BlockSpec(memory_space=pl.ANY)
    return pl.pallas_call(
        body,
        out_shape=jax.ShapeDtypeStruct((B, 8), BF16),
        in_specs=[any_space] * 15,
        out_specs=pl.BlockSpec(memory_space=pltpu.VMEM),
        scratch_shapes=scratch,
        compiler_params=pltpu.CompilerParams(
            collective_id=0, has_side_effects=True, vmem_limit_bytes=48 * 1024 * 1024
        ),
        name="step",
    )(
        tokens, w_query, w_key, w_value, w_forget, w_out,
        mix_gain.reshape(1, 8), mix_bias.reshape(1, 8),
        ffn_gain.reshape(1, 8), ffn_bias.reshape(1, 8),
        w_up, down_weight,
        cache_keys.reshape(B, POS, HEAD_DIM), cache_values.reshape(B, POS, HEAD_DIM),
        cum_gates,
    )


def solution(mesh):
    finer = Mesh(mesh.devices.reshape(NZ, NX, NY, NC), ("z", "x", "y", "c"))
    kv, tp, both = ("z", "x"), ("y", "c"), ("z", "x", "y", "c")
    return jax.shard_map(
        shards,
        mesh=finer,
        in_specs=(
            P(None, both), P(kv, tp), P(kv, tp), P(kv, tp), P(), P(tp, kv),
            P(both), P(both), P(both), P(both),
            P(kv, tp), P(tp, kv),
            P(None, tp, kv, None), P(None, tp, kv, None), P(None, tp, kv),
        ),
        out_specs=P(None, both),
        check_vma=False,
    )
```

```python
import jax
import jax.numpy as jnp
from jax import lax
from jax.experimental import pallas as pl
from jax.experimental.pallas import tpu as pltpu
from jax.sharding import Mesh
from jax.sharding import PartitionSpec as P

D = 2048
HEAD_DIM = 128
B = 16
POS = 512
NZ, NX, NY, NC = 8, 4, 4, 2
NKV, NTP = NZ * NX, NY * NC
ROOT2 = 1.4142135623730951
EPS = 1e-05
SCALE = HEAD_DIM**-0.5
F32 = jnp.float32
BF16 = jnp.bfloat16
MESH = pl.DeviceIdType.MESH


def across(a, b):
    return lax.dot_general(a, b, (((1,), (1,)), ((), ())), preferred_element_type=F32)


def body(
    tokens, w_query, w_key, w_value, w_forget, w_out, mix_gain, mix_bias, ffn_gain, ffn_bias,
    w_up, w_down, keys, values, gates,
    out,
    tok_v, gain_v, bias_v, fgain_v, fbias_v, wq_v, wkv_v, wf_v, wo_v, wup_v, wdn_v, k_v, v_v, cg_v,
    stage, plane, q_buf, kvg_send, kvg_buf, gwb_send, gwb_buf, accx, stx, accz, stz, head_buf,
    mst, up_send, up_buf, hid_buf, hid_f, down_buf, ost, turned,
    load_sem, k_sem, v_sem, send_sem, recv_sem,
):
    z, x, y, c = (lax.axis_index(a) for a in ("z", "x", "y", "c"))
    kv = z * NX + x
    tp = y * NC + c
    slot = x * NTP + tp

    barrier = pltpu.get_barrier_semaphore()

    def plane_peer(i):
        t = i // NTP
        r = i % NTP
        px = (x + NX - 1 - t + NX) % NX
        py = (y + NY - 1 - r // NC + NY) % NY
        pc = (c + NC - 1 - r % NC) % NC
        return {"x": px, "y": py, "c": pc}

    def greet_plane(i, carry):
        pl.semaphore_signal(barrier, inc=1, device_id=plane_peer(i), device_id_type=MESH)
        return carry

    def greet_line(i, carry):
        pl.semaphore_signal(
            barrier, inc=1, device_id={"z": (z + 1 + i) % NZ}, device_id_type=MESH
        )
        return carry

    lax.fori_loop(0, NZ - 1, greet_line, 0)
    lax.fori_loop(0, NX * NTP - 1, greet_plane, 0)

    loads = []

    def load(src, dst, sem):
        copy = pltpu.make_async_copy(src, dst, sem)
        copy.start()
        return copy

    first = [
        load(tokens, tok_v, load_sem.at[0]),
        load(mix_gain, gain_v, load_sem.at[1]),
        load(mix_bias, bias_v, load_sem.at[2]),
    ]
    load_q = load(w_query, wq_v.at[x], load_sem.at[3])
    load_k = load(w_key, wkv_v.at[x, 0], load_sem.at[4])
    load_v = load(w_value, wkv_v.at[x, 1], load_sem.at[5])
    load_f = load(w_forget.at[:, pl.ds(z * NX * 64, NX * 64)], wf_v, load_sem.at[6])
    load_o = load(w_out, wo_v, load_sem.at[7])
    load_up = load(w_up, wup_v, load_sem.at[8])
    load_fg = load(ffn_gain, fgain_v, load_sem.at[9])
    load_fb = load(ffn_bias, fbias_v, load_sem.at[10])
    load_cg = load(gates, cg_v, load_sem.at[11])
    load_key = [load(keys.at[pl.ds(4 * i, 4)], k_v.at[pl.ds(4 * i, 4)], k_sem.at[i]) for i in range(4)]
    load_val = [load(values.at[pl.ds(4 * i, 4)], v_v.at[pl.ds(4 * i, 4)], v_sem.at[i]) for i in range(4)]
    load_dn = load(w_down, wdn_v, load_sem.at[12])

    lane = lax.broadcasted_iota(jnp.int32, (B, 128), 1)
    row = lax.broadcasted_iota(jnp.int32, (B, 128), 0)
    lane1 = lax.broadcasted_iota(jnp.int32, (1, 128), 1)
    diag = row == lane
    diag16 = row == lane - B

    def to_row(col, mask):
        return jnp.sum(jnp.where(mask, jnp.broadcast_to(col, (B, 128)), 0.0), axis=0, keepdims=True)

    def to_col(line):
        return jnp.sum(
            jnp.where(diag, jnp.broadcast_to(line, (B, 128)), 0.0), axis=1, keepdims=True
        )

    for copy in first:
        copy.wait()
    lane_8 = lax.broadcasted_iota(jnp.int32, (8, 128), 1)
    diag_8 = lax.broadcasted_iota(jnp.int32, (8, 8), 0) == lax.broadcasted_iota(
        jnp.int32, (8, 8), 1
    )

    def upright(line):
        return jnp.sum(
            jnp.where(diag_8, jnp.broadcast_to(line, (8, 8)), 0.0), axis=1, keepdims=True
        )

    stage[...] = jnp.where(
        lane_8 == B, upright(gain_v[...]), jnp.where(lane_8 == B + 1, upright(bias_v[...]), 0.0)
    )
    stage[:, 0:B] = tok_v[...].astype(F32)
    plane[slot] = stage[...]
    load_q.wait()
    load_k.wait()
    load_v.wait()

    pl.semaphore_wait(barrier, NZ - 1 + NX * NTP - 1)

    def push(src, dst, phase, peer):
        pltpu.make_async_remote_copy(
            src_ref=src,
            dst_ref=dst,
            send_sem=send_sem.at[phase],
            recv_sem=recv_sem.at[phase],
            device_id=peer,
            device_id_type=MESH,
        ).start()

    def received(ref, count, phase):
        part = ref.at[pl.ds(0, count)]
        pltpu.make_async_copy(part, part, recv_sem.at[phase]).wait()

    def sent(ref, count, phase):
        part = ref.at[pl.ds(0, count)]
        pltpu.make_async_copy(part, part, send_sem.at[phase]).wait()

    def line_peer(i):
        step = (i + 1) // 2 * (2 * (i % 2) - 1) + 4
        return (z + step + NZ) % NZ

    def kv_peer(i):
        t = i // NX
        step = (t + 1) // 2 * (2 * (t % 2) - 1) + 4
        return (z + step + NZ) % NZ, (x + NX - 1 - i % NX) % NX

    def loop(count, f):
        def step(i, carry):
            f(i)
            return carry

        lax.fori_loop(0, count, step, 0)

    loop(NX * NTP - 1, lambda i: push(plane.at[slot], plane.at[slot], 0, plane_peer(i)))
    loop(NX - 1, lambda i: push(wq_v.at[x], wq_v.at[x], 1, {"x": (x + NX - 1 - i) % NX}))
    loop(NX - 1, lambda i: push(wkv_v.at[x], wkv_v.at[x], 2, {"x": (x + NX - 1 - i) % NX}))

    received(plane, NX * NTP - 1, 0)
    spread = plane[...].reshape(NX * NTP * 8, 128).T
    tok = spread[0:B, :].astype(BF16)
    received(wq_v, NX - 1, 1)
    q_buf[z] = jnp.dot(tok, wq_v[...].reshape(NX * 64, HEAD_DIM), preferred_element_type=F32)
    loop(
        NZ - 1, lambda i: push(q_buf.at[z], q_buf.at[z], 3, {"z": line_peer(i)})
    )
    received(wkv_v, NX - 1, 2)
    load_f.wait()
    key_part = jnp.dot(tok, wkv_v[:, 0].reshape(NX * 64, HEAD_DIM), preferred_element_type=F32)
    value_part = jnp.dot(tok, wkv_v[:, 1].reshape(NX * 64, HEAD_DIM), preferred_element_type=F32)
    gate_part = across(tok, wf_v[...])
    lane8 = lax.broadcasted_iota(jnp.int32, (B, 8), 1)
    gate_part = jnp.sum(jnp.where(lane8 == tp, gate_part, 0.0), axis=1, keepdims=True)
    gate_part = jnp.broadcast_to(gate_part, (B, 128))
    for i in range(NZ):
        kvg_send[i, :, 0:128] = key_part[2 * i : 2 * i + 2, :]
        kvg_send[i, :, 128:256] = value_part[2 * i : 2 * i + 2, :]
        kvg_send[i, :, 256:384] = gate_part[2 * i : 2 * i + 2, :]
    kvg_buf[z] = kvg_send[z]

    def push_kvg(i):
        pz = line_peer(i)
        push(kvg_send.at[pz], kvg_buf.at[z], 4, {"z": pz})

    loop(NZ - 1, push_kvg)

    own = jnp.where(x >= 2, spread[0:24, 128:256], spread[0:24, 0:128])
    own = jnp.where(x % 2 == 1, pltpu.roll(own, 64, 1), own)
    tok_own = own[0:B, :]
    gain_own = own[B : B + 1, :]
    bias_own = own[B + 1 : B + 2, :]

    load_up.wait()
    both = jnp.concatenate([gain_own, bias_own], axis=0)[:, 0:64]
    both_hi = both.astype(BF16)
    both_lo = (both - both_hi.astype(F32)).astype(BF16)
    gwb = jnp.dot(
        jnp.concatenate([both_hi.astype(F32), both_lo.astype(F32)], axis=0).astype(BF16),
        wup_v[...],
        preferred_element_type=F32,
    )
    gwb = gwb[0:2, :] + gwb[2:4, :]
    for h in range(2):
        for j in range(4):
            at = (h * 4 + j) * 128
            gwb_send[h, j : j + 1, :] = gwb[0:1, at : at + 128]
            gwb_send[h, 4 + j : 5 + j, :] = gwb[1:2, at : at + 128]
    gwb_buf[kv] = gwb_send[kv % 2]

    received(q_buf, NZ - 1, 3)
    query = jnp.sum(q_buf[...], axis=0).astype(BF16)

    def push_gwb(i):
        pz, px = kv_peer(i)
        push(gwb_send.at[px % 2], gwb_buf.at[kv], 5, {"z": pz, "x": px})

    loop(NKV - 1, push_gwb)

    load_cg.wait()
    row_pos = lax.broadcasted_iota(jnp.int32, (B, POS), 0)
    scores = jnp.zeros((B, POS), F32)
    for b in range(B):
        if b % 4 == 0:
            load_key[b // 4].wait()
        part = across(query, k_v[b])
        scores = jnp.where(row_pos == b, part, scores)
    gates_here = jnp.concatenate([cg_v[b] for b in range(B)], axis=0)
    scores = scores * SCALE + gates_here
    received(kvg_buf, NZ - 1, 4)
    kvg = jnp.sum(kvg_buf[...], axis=0)
    kvg16 = jnp.where(
        lax.broadcasted_iota(jnp.int32, (B, 384), 0) % 2 == 0,
        jnp.broadcast_to(kvg[0:1, :], (B, 384)),
        jnp.broadcast_to(kvg[1:2, :], (B, 384)),
    )
    key_new = kvg16[:, 0:128].astype(BF16).astype(F32)
    value_new = kvg16[:, 128:256].astype(BF16).astype(F32)
    gate_sum = kvg16[:, 256:257]
    log_forget = jnp.minimum(gate_sum, 0.0) - jnp.log1p(jnp.exp(-jnp.abs(gate_sum)))
    own_score = jnp.sum(query.astype(F32) * key_new, axis=1, keepdims=True) * SCALE - log_forget
    mine = (row[:, 0:1] // 2 == z) & (x == 0)
    own_score = jnp.where(mine, own_score, -1e30)
    value_new = jnp.where(mine, value_new, 0.0)
    peak = jnp.maximum(jnp.max(scores, axis=1, keepdims=True), own_score)
    weights = jnp.exp(scores - peak)
    own_weight = jnp.exp(own_score - peak)
    total = jnp.sum(weights, axis=1, keepdims=True) + own_weight
    weights = weights.astype(BF16)
    acc = jnp.zeros((B, HEAD_DIM), F32)
    for b in range(B):
        if b % 4 == 0:
            load_val[b // 4].wait()
        part = jnp.dot(weights, v_v[b], preferred_element_type=F32)
        acc = jnp.where(row == b, part, acc)
    acc = acc + own_weight * value_new

    stx[x] = jnp.concatenate([to_row(peak, diag), to_row(total, diag)], axis=0)
    loop(NX - 1, lambda i: push(stx.at[x], stx.at[x], 7, {"x": (x + NX - 1 - i) % NX}))
    accx[x] = acc
    loop(NX - 1, lambda i: push(accx.at[x], accx.at[x], 6, {"x": (x + NX - 1 - i) % NX}))

    def combine(acc_ref, st_ref, count, acc_phase, st_phase):
        received(st_ref, count - 1, st_phase)
        peaks = [st_ref[i, 0:1, :] for i in range(count)]
        peak = peaks[0]
        for p in peaks[1:]:
            peak = jnp.maximum(peak, p)
        factors = [jnp.exp(p - peak) for p in peaks]
        total = factors[0] * st_ref[0, 1:2, :]
        for i in range(1, count):
            total = total + factors[i] * st_ref[i, 1:2, :]
        cols = [to_col(f) for f in factors]
        received(acc_ref, count - 1, acc_phase)
        acc = cols[0] * acc_ref[0]
        for i in range(1, count):
            acc = acc + cols[i] * acc_ref[i]
        return peak, total, acc

    load_o.wait()
    w_out2 = jnp.concatenate([wo_v[...], wo_v[...]], axis=0)
    load_dn.wait()
    w_down2 = jnp.concatenate([wdn_v[...], wdn_v[...]], axis=0)

    peak, total, acc = combine(accx, stx, NX, 6, 7)
    stz[z] = jnp.concatenate([peak, total], axis=0)
    loop(NZ - 1, lambda i: push(stz.at[z], stz.at[z], 9, {"z": line_peer(i)}))
    accz[z] = acc
    loop(NZ - 1, lambda i: push(accz.at[z], accz.at[z], 8, {"z": line_peer(i)}))
    peak, total, acc = combine(accz, stz, NZ, 8, 9)
    attended = (acc / to_col(total)).astype(BF16)

    lane_half = lax.broadcasted_iota(jnp.int32, (8, 128), 1) < 64

    def tp_peer(i):
        return {"y": (y + NY - 1 - i // NC) % NY, "c": (c + NC - 1 - i % NC) % NC}

    def tp_sum(terms, ref, phase):
        ref[tp] = jnp.where(lane_half, terms[0:8, :], terms[8:16, :])
        loop(NTP - 1, lambda i: push(ref.at[tp], ref.at[tp], phase, tp_peer(i)))
        received(ref, NTP - 1, phase)
        summed = jnp.sum(ref[...], axis=0)
        return jnp.concatenate([summed, pltpu.roll(summed, 64, 1)], axis=0)

    head_terms = tp_sum(across(attended, w_out2), head_buf, 10)
    mixed = jnp.where(lane < 64, ROOT2 * tok_own + head_terms, 0.0)

    def push_stats(values, ref, phase):
        sums = jnp.sum(values, axis=1, keepdims=True)
        squares = jnp.sum(values * values, axis=1, keepdims=True)
        ref[kv] = to_row(sums, diag) + to_row(squares, diag16)

        def push_one(i):
            pz, px = kv_peer(i)
            push(ref.at[kv], ref.at[kv], phase, {"z": pz, "x": px})

        loop(NKV - 1, push_one)

    def stats(ref, phase):
        received(ref, NKV - 1, phase)
        line = jnp.sum(ref[...], axis=0)
        mean = line / D
        var = pltpu.roll(line, 128 - B, 1) / D - mean * mean
        return mean, lax.rsqrt(var + EPS)

    push_stats(mixed, mst, 11)

    scaled = mixed * jnp.broadcast_to(gain_own, (B, 128))
    scaled_hi = scaled.astype(BF16)
    scaled_lo = (scaled - scaled_hi.astype(F32)).astype(BF16)
    up = jnp.dot(
        jnp.concatenate([scaled_hi, scaled_lo], axis=0)[:, 0:64],
        wup_v[...],
        preferred_element_type=F32,
    )
    up = up[0:B, :] + up[B : 2 * B, :]
    for h in range(2):
        for j in range(4):
            at = (h * 4 + j) * 128
            up_send[:, h, j, :] = up[:, at : at + 128]
    up_buf[kv] = up_send[kv // 2, kv % 2]

    def push_up(i):
        pz, px = kv_peer(i)
        push(up_send.at[2 * pz + px // 2, px % 2], up_buf.at[kv], 12, {"z": pz, "x": px})

    loop(NKV - 1, push_up)
    received(gwb_buf, NKV - 1, 5)
    gwb = jnp.sum(gwb_buf[...], axis=0)
    mean, rstd = stats(mst, 11)
    pick = lane1 == kv // 2
    mean_here = jnp.sum(jnp.where(pick, mean, 0.0), axis=1, keepdims=True)
    rstd_here = jnp.sum(jnp.where(pick, rstd, 0.0), axis=1, keepdims=True)
    received(up_buf, NKV - 1, 12)
    up_sum = jnp.sum(up_buf[...], axis=0)
    up_row = rstd_here * (up_sum - mean_here * gwb[0:4, :]) + gwb[4:8, :]
    hidden = jnp.square(jnp.maximum(up_row, 0.0)).astype(BF16)
    hid_buf[kv] = hidden

    def push_hidden(i):
        pz, px = kv_peer(i)
        push(hid_buf.at[kv], hid_buf.at[kv], 13, {"z": pz, "x": px})

    loop(NKV - 1, push_hidden)

    normed = (mixed - to_col(mean)) * to_col(rstd) * gain_own + bias_own
    normed = normed.astype(BF16).astype(F32)
    received(hid_buf, NKV - 1, 13)
    hid_f[...] = hid_buf[...].astype(F32).reshape(B, 2, 4, 128)
    hidden_all = jnp.concatenate(
        [hid_f[:, h, j, :].astype(BF16) for h in range(2) for j in range(4)], axis=1
    )
    down_terms = tp_sum(across(hidden_all, w_down2), down_buf, 14)
    outer = jnp.where(lane < 64, ROOT2 * normed + down_terms, 0.0)
    push_stats(outer, ost, 15)
    turned[...] = jnp.concatenate([outer, jnp.zeros((128 - B, 128), F32)], axis=0).T
    outer = turned[pl.ds(8 * tp, 8), 0:B]
    load_fg.wait()
    load_fb.wait()
    fgain = upright(fgain_v[...])
    fbias = upright(fbias_v[...])

    sent(plane, NX * NTP - 1, 0)
    sent(wq_v, NX - 1, 1)
    sent(wkv_v, NX - 1, 2)
    sent(q_buf, NZ - 1, 3)
    sent(kvg_buf, NZ - 1, 4)
    sent(gwb_buf, NKV - 1, 5)
    sent(accx, NX - 1, 6)
    sent(stx, NX - 1, 7)
    sent(accz, NZ - 1, 8)
    sent(stz, NZ - 1, 9)
    sent(head_buf, NTP - 1, 10)
    sent(mst, NKV - 1, 11)
    sent(up_buf, NKV - 1, 12)
    sent(hid_buf, NKV - 1, 13)
    sent(down_buf, NTP - 1, 14)
    sent(ost, NKV - 1, 15)
    mean, rstd = stats(ost, 15)
    result = (outer - mean[:, 0:B]) * rstd[:, 0:B] * fgain + fbias
    out[...] = result.astype(BF16)


def shards(
    tokens, w_query, w_key, w_value, w_forget, w_out, mix_gain, mix_bias, ffn_gain, ffn_bias,
    w_up, down_weight, cache_keys, cache_values, cum_gates,
):
    vmem = pltpu.VMEM
    scratch = [
        vmem((8, B), BF16),
        vmem((1, 8), F32),
        vmem((1, 8), F32),
        vmem((1, 8), F32),
        vmem((1, 8), F32),
        vmem((NX, 64, 128), BF16),
        vmem((NX, 2, 64, 128), BF16),
        vmem((8, NX * 64), BF16),
        vmem((64, 128), BF16),
        vmem((64, 1024), BF16),
        vmem((64, 1024), BF16),
        vmem((B, POS, 128), BF16),
        vmem((B, POS, 128), BF16),
        vmem((B, 1, POS), F32),
        vmem((8, 128), F32),
        vmem((NX * NTP, 8, 128), F32),
        vmem((NZ, B, 128), F32),
        vmem((NZ, 2, 384), F32),
        vmem((NZ, 2, 384), F32),
        vmem((2, 8, 128), F32),
        vmem((NKV, 8, 128), F32),
        vmem((NX, B, 128), F32),
        vmem((NX, 2, 128), F32),
        vmem((NZ, B, 128), F32),
        vmem((NZ, 2, 128), F32),
        vmem((NTP, 8, 128), F32),
        vmem((NKV, 1, 128), F32),
        vmem((B, 2, 4, 128), F32),
        vmem((NKV, 4, 128), F32),
        vmem((NKV, 4, 128), BF16),
        vmem((B, 2, 4, 128), F32),
        vmem((NTP, 8, 128), F32),
        vmem((NKV, 1, 128), F32),
        vmem((128, 128), F32),
        pltpu.SemaphoreType.DMA((13,)),
        pltpu.SemaphoreType.DMA((4,)),
        pltpu.SemaphoreType.DMA((4,)),
        pltpu.SemaphoreType.DMA((16,)),
        pltpu.SemaphoreType.DMA((16,)),
    ]
    any_space = pl.BlockSpec(memory_space=pltpu.HBM)
    return pl.pallas_call(
        body,
        out_shape=jax.ShapeDtypeStruct((8, B), BF16),
        in_specs=[any_space] * 15,
        out_specs=pl.BlockSpec(memory_space=pltpu.VMEM),
        scratch_shapes=scratch,
        compiler_params=pltpu.CompilerParams(
            collective_id=0, has_side_effects=True, vmem_limit_bytes=67043328
        ),
        name="step",
    )(
        tokens.T, w_query, w_key, w_value, w_forget.T, w_out.T,
        mix_gain.reshape(1, 8), mix_bias.reshape(1, 8),
        ffn_gain.reshape(1, 8), ffn_bias.reshape(1, 8),
        w_up, down_weight.T,
        cache_keys.reshape(B, POS, HEAD_DIM), cache_values.reshape(B, POS, HEAD_DIM),
        cum_gates,
    ).T


def solution(mesh):
    finer = Mesh(mesh.devices.reshape(NZ, NX, NY, NC), ("z", "x", "y", "c"))
    kv, tp, both = ("z", "x"), ("y", "c"), ("z", "x", "y", "c")
    return jax.shard_map(
        shards,
        mesh=finer,
        in_specs=(
            P(None, both), P(kv, tp), P(kv, tp), P(kv, tp), P(), P(tp, kv),
            P(both), P(both), P(both), P(both),
            P(kv, tp), P(tp, kv),
            P(None, tp, kv, None), P(None, tp, kv, None), P(None, tp, kv),
        ),
        out_specs=P(None, both),
        check_vma=False,
    )
```

```python
import jax
import jax.numpy as jnp
from jax import lax
from jax.experimental import pallas as pl
from jax.experimental.pallas import tpu as pltpu
from jax.sharding import Mesh
from jax.sharding import PartitionSpec as P

D = 2048
HEAD_DIM = 128
B = 16
POS = 512
NZ, NX, NY, NC = 8, 4, 4, 2
NKV, NTP = NZ * NX, NY * NC
ROOT2 = 1.4142135623730951
EPS = 1e-05
SCALE = HEAD_DIM**-0.5
F32 = jnp.float32
BF16 = jnp.bfloat16
MESH = pl.DeviceIdType.MESH


def across(a, b):
    return lax.dot_general(a, b, (((1,), (1,)), ((), ())), preferred_element_type=F32)


def body(
    tokens, w_query, w_key, w_value, w_forget, w_out, mix_gain, mix_bias, ffn_gain, ffn_bias,
    w_up, w_down, keys, values, gates,
    out,
    tok_v, gain_v, bias_v, fgain_v, fbias_v, wq_v, wkv_v, wf_v, wo_v, wup_v, wdn_v, k_v, v_v, cg_v,
    gb_buf, plane, q_buf, kvg_send, kvg_buf, gwb_send, gwb_buf, accx, stx, accz, stz, head_buf,
    mst, up_send, up_buf, hid_buf, hid_f, down_buf, ost, turned,
    load_sem, k_sem, v_sem, send_sem, recv_sem,
):
    z, x, y, c = (lax.axis_index(a) for a in ("z", "x", "y", "c"))
    kv = z * NX + x
    tp = y * NC + c
    slot = x * NTP + tp

    barrier = pltpu.get_barrier_semaphore()

    xs = [x] + [lax.rem(x + i, NX) for i in range(1, NX)]
    ys = [y] + [lax.rem(y + i, NY) for i in range(1, NY)]
    cs = [c, 1 - c]
    zs = [z] + [lax.rem(z + i, NZ) for i in range(1, NZ)]
    line = (4, 3, 5, 2, 6, 1, 7)
    ring = (2, 1, 3)
    x_peers = [{"x": xs[i]} for i in ring]
    z_peers = [{"z": zs[i]} for i in line]
    tp_peers = [{"y": ys[i], "c": cs[j]} for i in ring for j in (1, 0)] + [{"c": cs[1]}]
    offsets = [(i, j, k) for i in (0, 2, 1, 3) for j in (0, 2, 1, 3) for k in (1, 0)]
    far = {0: 0, 1: 1, 2: 2, 3: 1}
    offsets = sorted(offsets, key=lambda o: -(far[o[0]] + far[o[1]]))[:-2] + [(0, 0, 1)]
    plane_peers = [{"x": xs[i], "y": ys[j], "c": cs[k]} for i, j, k in offsets]
    pairs = sorted(
        [(i, j) for i in range(NZ) for j in range(NX) if i or j],
        key=lambda o: -(min(o[0], NZ - o[0]) + far[o[1]]),
    )
    kv_peers = [{"z": zs[i], "x": xs[j]} for i, j in pairs]

    for peer in z_peers + plane_peers:
        pl.semaphore_signal(barrier, inc=1, device_id=peer, device_id_type=MESH)

    loads = []

    def load(src, dst, sem):
        copy = pltpu.make_async_copy(src, dst, sem)
        copy.start()
        return copy

    first = [
        load(tokens, tok_v, load_sem.at[0]),
        load(mix_gain, gain_v, load_sem.at[1]),
        load(mix_bias, bias_v, load_sem.at[2]),
    ]
    load_q = load(w_query, wq_v.at[x], load_sem.at[3])
    load_k = load(w_key, wkv_v.at[x, 0], load_sem.at[4])
    load_v = load(w_value, wkv_v.at[x, 1], load_sem.at[5])
    load_f = load(w_forget.at[:, pl.ds(z * NX * 64, NX * 64)], wf_v, load_sem.at[6])
    load_o = [load(w_out, wo_v.at[pl.ds(64 * i, 64)], load_sem.at[7 + 6 * i]) for i in range(2)]
    load_up = load(w_up, wup_v, load_sem.at[8])
    load_fg = load(ffn_gain, fgain_v, load_sem.at[9])
    load_fb = load(ffn_bias, fbias_v, load_sem.at[10])
    load_cg = load(gates, cg_v, load_sem.at[11])
    load_key = [load(keys.at[pl.ds(4 * i, 4)], k_v.at[pl.ds(4 * i, 4)], k_sem.at[i]) for i in range(4)]
    load_val = [load(values.at[pl.ds(4 * i, 4)], v_v.at[pl.ds(4 * i, 4)], v_sem.at[i]) for i in range(4)]
    load_dn = [load(w_down, wdn_v.at[pl.ds(64 * i, 64)], load_sem.at[12 + 2 * i]) for i in range(2)]

    lane = lax.broadcasted_iota(jnp.int32, (B, 128), 1)
    row = lax.broadcasted_iota(jnp.int32, (B, 128), 0)
    lane1 = lax.broadcasted_iota(jnp.int32, (1, 128), 1)
    diag = row == lane
    diag16 = row == lane - B

    def to_row(col, mask):
        return jnp.sum(jnp.where(mask, jnp.broadcast_to(col, (B, 128)), 0.0), axis=0, keepdims=True)

    def to_col(line):
        return jnp.sum(
            jnp.where(diag, jnp.broadcast_to(line, (B, 128)), 0.0), axis=1, keepdims=True
        )

    for copy in first:
        copy.wait()
    plane[slot, :, 0:B] = tok_v[...]
    lane_8 = lax.broadcasted_iota(jnp.int32, (8, 128), 1)
    diag_8 = lax.broadcasted_iota(jnp.int32, (8, 8), 0) == lax.broadcasted_iota(
        jnp.int32, (8, 8), 1
    )

    def upright(line):
        return jnp.sum(
            jnp.where(diag_8, jnp.broadcast_to(line, (8, 8)), 0.0), axis=1, keepdims=True
        )

    gb_buf[tp] = jnp.where(
        lane_8 == 0, upright(gain_v[...]), jnp.where(lane_8 == 1, upright(bias_v[...]), 0.0)
    )
    load_q.wait()
    load_k.wait()
    load_v.wait()

    pl.semaphore_wait(barrier, NZ - 1 + NX * NTP - 1)

    def push(src, dst, phase, peer):
        pltpu.make_async_remote_copy(
            src_ref=src,
            dst_ref=dst,
            send_sem=send_sem.at[phase],
            recv_sem=recv_sem.at[phase],
            device_id=peer,
            device_id_type=MESH,
        ).start()

    def received(ref, count, phase):
        part = ref.at[pl.ds(0, count)]
        pltpu.make_async_copy(part, part, recv_sem.at[phase]).wait()

    def sent(ref, count, phase):
        part = ref.at[pl.ds(0, count)]
        pltpu.make_async_copy(part, part, send_sem.at[phase]).wait()

    def spread_out(ref, phase, peers):
        for peer in peers:
            push(ref, ref, phase, peer)

    spread_out(plane.at[slot], 0, plane_peers)
    spread_out(wq_v.at[x], 1, x_peers)
    spread_out(wkv_v.at[x], 2, x_peers)
    spread_out(gb_buf.at[tp], 16, tp_peers)

    received(plane, NX * NTP - 1, 0)
    spread = plane[...].astype(F32).reshape(NX * NTP * 8, 128).T
    tok = spread[0:B, :].astype(BF16)
    received(wq_v, NX - 1, 1)
    q_buf[z] = jnp.dot(tok, wq_v[...].reshape(NX * 64, HEAD_DIM), preferred_element_type=F32)
    spread_out(q_buf.at[z], 3, z_peers)
    received(wkv_v, NX - 1, 2)
    load_f.wait()
    key_part = jnp.dot(tok, wkv_v[:, 0].reshape(NX * 64, HEAD_DIM), preferred_element_type=F32)
    value_part = jnp.dot(tok, wkv_v[:, 1].reshape(NX * 64, HEAD_DIM), preferred_element_type=F32)
    gate_part = across(tok, wf_v[...])
    lane8 = lax.broadcasted_iota(jnp.int32, (B, 8), 1)
    gate_part = jnp.sum(jnp.where(lane8 == tp, gate_part, 0.0), axis=1, keepdims=True)
    gate_part = jnp.broadcast_to(gate_part, (B, 128))
    for i in range(NZ):
        kvg_send[i, :, 0:128] = key_part[2 * i : 2 * i + 2, :]
        kvg_send[i, :, 128:256] = value_part[2 * i : 2 * i + 2, :]
        kvg_send[i, :, 256:384] = gate_part[2 * i : 2 * i + 2, :]
    kvg_buf[z] = kvg_send[z]
    for peer in z_peers:
        push(kvg_send.at[peer["z"]], kvg_buf.at[z], 4, peer)

    own = jnp.where(x >= 2, spread[0:B, 128:256], spread[0:B, 0:128])
    tok_own = jnp.where(x % 2 == 1, pltpu.roll(own, 64, 1), own)
    received(gb_buf, NTP - 1, 16)
    both = jnp.concatenate(
        [gb_buf[...].reshape(64, 128), jnp.zeros((64, 128), F32)], axis=0
    ).T
    gain_own = both[0:1, :]
    bias_own = both[1:2, :]

    load_up.wait()
    both = both[0:2, 0:64]
    both_hi = both.astype(BF16)
    both_lo = (both - both_hi.astype(F32)).astype(BF16)
    gwb = jnp.dot(
        jnp.concatenate([both_hi.astype(F32), both_lo.astype(F32)], axis=0).astype(BF16),
        wup_v[...],
        preferred_element_type=F32,
    )
    gwb = gwb[0:2, :] + gwb[2:4, :]
    for h in range(2):
        for j in range(4):
            at = (h * 4 + j) * 128
            gwb_send[h, j : j + 1, :] = gwb[0:1, at : at + 128]
            gwb_send[h, 4 + j : 5 + j, :] = gwb[1:2, at : at + 128]
    gwb_buf[kv] = gwb_send[kv % 2]

    for peer in kv_peers:
        push(gwb_send.at[lax.rem(peer["x"], 2)], gwb_buf.at[kv], 5, peer)

    received(q_buf, NZ - 1, 3)
    query = jnp.sum(q_buf[...], axis=0).astype(BF16)

    load_cg.wait()
    row_pos = lax.broadcasted_iota(jnp.int32, (B, POS), 0)
    scores = jnp.zeros((B, POS), F32)
    for b in range(B):
        if b % 4 == 0:
            load_key[b // 4].wait()
        part = across(query, k_v[b])
        scores = jnp.where(row_pos == b, part, scores)
    gates_here = jnp.concatenate([cg_v[b] for b in range(B)], axis=0)
    scores = scores * SCALE + gates_here
    received(kvg_buf, NZ - 1, 4)
    kvg = jnp.sum(kvg_buf[...], axis=0)
    kvg16 = jnp.where(
        lax.broadcasted_iota(jnp.int32, (B, 384), 0) % 2 == 0,
        jnp.broadcast_to(kvg[0:1, :], (B, 384)),
        jnp.broadcast_to(kvg[1:2, :], (B, 384)),
    )
    key_new = kvg16[:, 0:128].astype(BF16).astype(F32)
    value_new = kvg16[:, 128:256].astype(BF16).astype(F32)
    gate_sum = kvg16[:, 256:257]
    log_forget = jnp.minimum(gate_sum, 0.0) - jnp.log1p(jnp.exp(-jnp.abs(gate_sum)))
    own_score = jnp.sum(query.astype(F32) * key_new, axis=1, keepdims=True) * SCALE - log_forget
    mine = (row[:, 0:1] // 2 == z) & (x == 0)
    own_score = jnp.where(mine, own_score, -1e30)
    value_new = jnp.where(mine, value_new, 0.0)
    peak = jnp.maximum(jnp.max(scores, axis=1, keepdims=True), own_score)
    weights = jnp.exp(scores - peak)
    own_weight = jnp.exp(own_score - peak)
    total = jnp.sum(weights, axis=1, keepdims=True) + own_weight
    weights = weights.astype(BF16)
    acc = jnp.zeros((B, HEAD_DIM), F32)
    for b in range(B):
        if b % 4 == 0:
            load_val[b // 4].wait()
        part = jnp.dot(weights, v_v[b], preferred_element_type=F32)
        acc = jnp.where(row == b, part, acc)
    acc = acc + own_weight * value_new

    stx[x] = jnp.concatenate([to_row(peak, diag), to_row(total, diag)], axis=0)
    spread_out(stx.at[x], 7, x_peers)
    accx[x] = acc
    spread_out(accx.at[x], 6, x_peers)

    def combine(acc_ref, st_ref, count, acc_phase, st_phase):
        received(st_ref, count - 1, st_phase)
        peaks = [st_ref[i, 0:1, :] for i in range(count)]
        peak = peaks[0]
        for p in peaks[1:]:
            peak = jnp.maximum(peak, p)
        factors = [jnp.exp(p - peak) for p in peaks]
        total = factors[0] * st_ref[0, 1:2, :]
        for i in range(1, count):
            total = total + factors[i] * st_ref[i, 1:2, :]
        cols = [to_col(f) for f in factors]
        received(acc_ref, count - 1, acc_phase)
        acc = cols[0] * acc_ref[0]
        for i in range(1, count):
            acc = acc + cols[i] * acc_ref[i]
        return peak, total, acc

    for copy in load_o + load_dn:
        copy.wait()
    peak, total, acc = combine(accx, stx, NX, 6, 7)
    stz[z] = jnp.concatenate([peak, total], axis=0)
    spread_out(stz.at[z], 9, z_peers)
    accz[z] = acc
    spread_out(accz.at[z], 8, z_peers)
    peak, total, acc = combine(accz, stz, NZ, 8, 9)
    attended = (acc / to_col(total)).astype(BF16)

    lane_half = lax.broadcasted_iota(jnp.int32, (8, 128), 1) < 64

    def tp_sum(terms, ref, phase):
        ref[tp] = jnp.where(lane_half, terms[0:8, :], terms[8:16, :])
        spread_out(ref.at[tp], phase, tp_peers)
        received(ref, NTP - 1, phase)
        summed = jnp.sum(ref[...], axis=0)
        return jnp.concatenate([summed, pltpu.roll(summed, 64, 1)], axis=0)

    head_terms = tp_sum(across(attended, wo_v[...]), head_buf, 10)
    mixed = jnp.where(lane < 64, ROOT2 * tok_own + head_terms, 0.0)

    def push_stats(values, ref, phase):
        sums = jnp.sum(values, axis=1, keepdims=True)
        squares = jnp.sum(values * values, axis=1, keepdims=True)
        ref[kv] = to_row(sums, diag) + to_row(squares, diag16)
        spread_out(ref.at[kv], phase, kv_peers)

    def stats(ref, phase):
        received(ref, NKV - 1, phase)
        line = jnp.sum(ref[...], axis=0)
        mean = line / D
        var = pltpu.roll(line, 128 - B, 1) / D - mean * mean
        return mean, lax.rsqrt(var + EPS)

    push_stats(mixed, mst, 11)

    scaled = mixed * jnp.broadcast_to(gain_own, (B, 128))
    scaled_hi = scaled.astype(BF16)
    scaled_lo = (scaled - scaled_hi.astype(F32)).astype(BF16)
    up = jnp.dot(
        jnp.concatenate([scaled_hi, scaled_lo], axis=0)[:, 0:64],
        wup_v[...],
        preferred_element_type=F32,
    )
    up = up[0:B, :] + up[B : 2 * B, :]
    for h in range(2):
        for j in range(4):
            at = (h * 4 + j) * 128
            up_send[:, h, j, :] = up[:, at : at + 128]
    up_buf[kv] = up_send[kv // 2, kv % 2]

    for peer in kv_peers:
        px = peer["x"]
        push(up_send.at[2 * peer["z"] + px // 2, lax.rem(px, 2)], up_buf.at[kv], 12, peer)
    received(gwb_buf, NKV - 1, 5)
    gwb = jnp.sum(gwb_buf[...], axis=0)
    mean, rstd = stats(mst, 11)
    pick = lane1 == kv // 2
    mean_here = jnp.sum(jnp.where(pick, mean, 0.0), axis=1, keepdims=True)
    rstd_here = jnp.sum(jnp.where(pick, rstd, 0.0), axis=1, keepdims=True)
    received(up_buf, NKV - 1, 12)
    up_sum = jnp.sum(up_buf[...], axis=0)
    up_row = rstd_here * (up_sum - mean_here * gwb[0:4, :]) + gwb[4:8, :]
    hidden = jnp.square(jnp.maximum(up_row, 0.0)).astype(BF16)
    hid_buf[kv] = hidden
    spread_out(hid_buf.at[kv], 13, kv_peers)

    normed = (mixed - to_col(mean)) * to_col(rstd) * gain_own + bias_own
    normed = normed.astype(BF16).astype(F32)
    received(hid_buf, NKV - 1, 13)
    hid_f[...] = hid_buf[...].astype(F32).reshape(B, 2, 4, 128)
    hidden_all = jnp.concatenate(
        [hid_f[:, h, j, :].astype(BF16) for h in range(2) for j in range(4)], axis=1
    )
    down_terms = tp_sum(across(hidden_all, wdn_v[...]), down_buf, 14)
    outer = jnp.where(lane < 64, ROOT2 * normed + down_terms, 0.0)
    push_stats(outer, ost, 15)
    turned[...] = jnp.concatenate([outer, jnp.zeros((128 - B, 128), F32)], axis=0).T
    outer = turned[pl.ds(8 * tp, 8), 0:B]
    load_fg.wait()
    load_fb.wait()
    fgain = upright(fgain_v[...])
    fbias = upright(fbias_v[...])

    sent(plane, NX * NTP - 1, 0)
    sent(wq_v, NX - 1, 1)
    sent(wkv_v, NX - 1, 2)
    sent(q_buf, NZ - 1, 3)
    sent(kvg_buf, NZ - 1, 4)
    sent(gwb_buf, NKV - 1, 5)
    sent(accx, NX - 1, 6)
    sent(stx, NX - 1, 7)
    sent(accz, NZ - 1, 8)
    sent(stz, NZ - 1, 9)
    sent(head_buf, NTP - 1, 10)
    sent(mst, NKV - 1, 11)
    sent(up_buf, NKV - 1, 12)
    sent(hid_buf, NKV - 1, 13)
    sent(down_buf, NTP - 1, 14)
    sent(ost, NKV - 1, 15)
    sent(gb_buf, NTP - 1, 16)
    mean, rstd = stats(ost, 15)
    result = (outer - mean[:, 0:B]) * rstd[:, 0:B] * fgain + fbias
    out[...] = result.astype(BF16)


def shards(
    tokens, w_query, w_key, w_value, w_forget, w_out, mix_gain, mix_bias, ffn_gain, ffn_bias,
    w_up, down_weight, cache_keys, cache_values, cum_gates,
):
    vmem = pltpu.VMEM
    scratch = [
        vmem((8, B), BF16),
        vmem((1, 8), F32),
        vmem((1, 8), F32),
        vmem((1, 8), F32),
        vmem((1, 8), F32),
        vmem((NX, 64, 128), BF16),
        vmem((NX, 2, 64, 128), BF16),
        vmem((8, NX * 64), BF16),
        vmem((128, 128), BF16),
        vmem((64, 1024), BF16),
        vmem((128, 1024), BF16),
        vmem((B, POS, 128), BF16),
        vmem((B, POS, 128), BF16),
        vmem((B, 1, POS), F32),
        vmem((NTP, 8, 128), F32),
        vmem((NX * NTP, 8, 128), BF16),
        vmem((NZ, B, 128), F32),
        vmem((NZ, 2, 384), F32),
        vmem((NZ, 2, 384), F32),
        vmem((2, 8, 128), F32),
        vmem((NKV, 8, 128), F32),
        vmem((NX, B, 128), F32),
        vmem((NX, 2, 128), F32),
        vmem((NZ, B, 128), F32),
        vmem((NZ, 2, 128), F32),
        vmem((NTP, 8, 128), F32),
        vmem((NKV, 1, 128), F32),
        vmem((B, 2, 4, 128), F32),
        vmem((NKV, 4, 128), F32),
        vmem((NKV, 4, 128), BF16),
        vmem((B, 2, 4, 128), F32),
        vmem((NTP, 8, 128), F32),
        vmem((NKV, 1, 128), F32),
        vmem((128, 128), F32),
        pltpu.SemaphoreType.DMA((15,)),
        pltpu.SemaphoreType.DMA((4,)),
        pltpu.SemaphoreType.DMA((4,)),
        pltpu.SemaphoreType.DMA((17,)),
        pltpu.SemaphoreType.DMA((17,)),
    ]
    any_space = pl.BlockSpec(memory_space=pltpu.HBM)
    return pl.pallas_call(
        body,
        out_shape=jax.ShapeDtypeStruct((8, B), BF16),
        in_specs=[any_space] * 15,
        out_specs=pl.BlockSpec(memory_space=pltpu.VMEM),
        scratch_shapes=scratch,
        compiler_params=pltpu.CompilerParams(
            collective_id=0, has_side_effects=True, vmem_limit_bytes=67043328
        ),
        name="step",
    )(
        tokens.T, w_query, w_key, w_value, w_forget.T, w_out.T,
        mix_gain.reshape(1, 8), mix_bias.reshape(1, 8),
        ffn_gain.reshape(1, 8), ffn_bias.reshape(1, 8),
        w_up, down_weight.T,
        cache_keys.reshape(B, POS, HEAD_DIM), cache_values.reshape(B, POS, HEAD_DIM),
        cum_gates,
    ).T


def solution(mesh):
    finer = Mesh(mesh.devices.reshape(NZ, NX, NY, NC), ("z", "x", "y", "c"))
    kv, tp, both = ("z", "x"), ("y", "c"), ("z", "x", "y", "c")
    return jax.shard_map(
        shards,
        mesh=finer,
        in_specs=(
            P(None, both), P(kv, tp), P(kv, tp), P(kv, tp), P(), P(tp, kv),
            P(both), P(both), P(both), P(both),
            P(kv, tp), P(tp, kv),
            P(None, tp, kv, None), P(None, tp, kv, None), P(None, tp, kv),
        ),
        out_specs=P(None, both),
        check_vma=False,
    )
```
